32 devices in a mesh: grp: 2 (over y), fs: 4 (over z), tp: 4 (over x, core).
Axes of the slice: x: 2, y: 2, z: 4, core: 2. Of those that a mesh axis runs over, the one named last changes fastest.
Arguments:
- tokens: bfloat16 [1024, 2048], P(('grp', 'fs')), parts along dimension 0, may hold values from -6 to 6
- pre_attention_gain: float32 [2048], replicated, may hold values from 0.1 to 1.9
- query_weight: bfloat16 [2048, 512], P('fs', 'tp'), may hold values from -0.125 to 0.125
- key_weight: bfloat16 [2048, 512], P('fs', 'tp'), may hold values from -0.125 to 0.125
- value_weight: bfloat16 [2048, 1024], P('fs', 'tp'), may hold values from -0.125 to 0.125
- output_gate_weight: bfloat16 [2048, 1024], P('fs', 'tp'), may hold values from -0.125 to 0.125
- decay_weight: bfloat16 [2048, 512], P('fs', 'tp'), may hold values from -0.25 to 0.25
- decay_logit_bias: float32 [512], P('tp'), may hold values from -1 to 4
- extra_log_decay: float32 [1024, 512], P(('grp', 'fs'), 'tp'), parts along dimension 0, may hold values from -0.7 to 0
- head_norm_gain: float32 [1024], P('tp'), may hold values from 0.1 to 1.9
- attention_out_weight: bfloat16 [1024, 2048], P('tp', 'fs'), may hold values from -0.1875 to 0.1875
- post_attention_gain: float32 [2048], replicated, may hold values from 0.1 to 1.9
- pre_feedforward_gain: float32 [2048], replicated, may hold values from 0.1 to 1.9
- post_feedforward_gain: float32 [2048], replicated, may hold values from 0.1 to 1.9
- up_weight: bfloat16 [2048, 8192], P('fs', 'tp'), may hold values from -0.125 to 0.125
- down_weight: bfloat16 [8192, 2048], P('tp', 'fs'), may hold values from -0.0625 to 0.0625
Outputs:
- layer_out: bfloat16 [1024, 2048], P(('grp', 'fs')), parts along dimension 0
The draws below stay inside these ranges and needn't reach their ends.
There are 2 independent parts, one for each index of `grp`. The reference program is written for one: setup_inputs(seed, part) draws one part's arguments, and reference() takes and returns one part's arrays. A program takes and returns all parts, laid end to end along the dimension named above; an argument that names none is the same for every part. Nothing has to cross between parts.
All inputs are finite; a program needn't handle non-finite values.
Results may differ from the reference program's by a relative error of at most 0.035.
Values may be sent and summed in bfloat16 or wider, within the bound.
A program may use at most 64 MiB of HBM per device.

```python
import jax
import jax.numpy as jnp
from jax import lax

D = 2048
HEADS = 8
DK = 64
DV = 128
BLOCK = 64
TOK_DEV = 128
QK = 512
V = 1024
FF = 8192
TOKENS = 512
N_TP = 4


def draw_extra_log_decay(key, part):
    first, second = jax.random.split(jax.random.fold_in(key, 11))
    chance = jax.random.uniform(first, (TOKENS, 1), jnp.float32)
    depth = jax.random.uniform(second, (TOKENS, QK), jnp.float32, minval=-0.7, maxval=-0.22)
    return jnp.where(chance < 3.0 / TOK_DEV, depth, 0.0).astype(jnp.float32)


def level_of(stream_key, extent, cuts, smallest, high):
    factor_of, own = 1.0, jax.random.fold_in(stream_key, 6)
    for axis_at, parts in cuts:
        heights = jnp.exp(jax.random.uniform(jax.random.fold_in(own, axis_at), (parts,), jnp.float32, smallest / len(cuts), high / len(cuts)))
        factor_of = factor_of * jnp.repeat(heights, extent[axis_at] // parts).reshape([-1 if axis == axis_at else 1 for axis in range(len(extent))])
    return factor_of


def scatter_about(own_key, shape, scale, limit, cuts=(), held_as=jnp.bfloat16):
    values = jax.random.normal(own_key, shape, jnp.float32) * scale
    if len(cuts) > 0:
        values = level_of(own_key, shape, cuts, -0.22, 0.18) * values
    return jnp.clip(values, min=-limit, max=limit).astype(held_as)


def setup_inputs(seed: int = 0, part: int = 0) -> dict:
    keys = jax.random.split(jax.random.key(seed), 17)
    own_keys = jax.random.split(jax.random.fold_in(keys[16], part), 17)
    return {
        "tokens": scatter_about(own_keys[0], (TOKENS, D), 1.0, 6.0, ((0, 4),)),
        "pre_attention_gain": jnp.clip(1.0 + 0.18 * jax.random.normal(keys[1], (D,), jnp.float32), 0.1, 1.9),
        "query_weight": scatter_about(keys[2], (D, QK), D ** -0.5, 0.125, ((0, 4), (1, 4))),
        "key_weight": scatter_about(keys[3], (D, QK), D ** -0.5, 0.125, ((0, 4), (1, 4))),
        "value_weight": scatter_about(keys[4], (D, V), D ** -0.5, 0.125, ((0, 4), (1, 4))),
        "output_gate_weight": scatter_about(keys[5], (D, V), D ** -0.5, 0.125, ((0, 4), (1, 4))),
        "decay_weight": scatter_about(keys[6], (D, QK), (D // 4) ** -0.5, 0.25, ((0, 4), (1, 4))),
        "decay_logit_bias": jnp.clip(-1.0 + 5.0 * jax.random.uniform(keys[7], (QK,), jnp.float32) ** level_of(keys[7], (QK,), ((0, 4),), -0.2, 0.2), -1.0, 4.0),
        "extra_log_decay": draw_extra_log_decay(jax.random.fold_in(jax.random.fold_in(keys[16], part), 71), part),
        "head_norm_gain": jnp.clip(1.0 + 0.18 * jax.random.normal(keys[9], (V,), jnp.float32), 0.1, 1.9),
        "attention_out_weight": scatter_about(keys[10], (V, D), V ** -0.5, 0.1875, ((0, 4), (1, 4))),
        "post_attention_gain": jnp.clip(1.0 + 0.18 * jax.random.normal(keys[11], (D,), jnp.float32), 0.1, 1.9),
        "pre_feedforward_gain": jnp.clip(1.0 + 0.18 * jax.random.normal(keys[12], (D,), jnp.float32), 0.1, 1.9),
        "post_feedforward_gain": jnp.clip(1.0 + 0.18 * jax.random.normal(keys[13], (D,), jnp.float32), 0.1, 1.9),
        "up_weight": scatter_about(keys[14], (D, FF), D ** -0.5, 0.125, ((0, 4), (1, 4))),
        "down_weight": scatter_about(keys[15], (FF, D), FF ** -0.5, 0.0625, ((0, 4), (1, 4))),
    }


EPS = 1e-06
GATE_NORM_SCALE = 16.0
HIGH = lax.Precision.HIGHEST

def root_norm(rows, gain):
    values = rows.astype(jnp.float32)
    return values * lax.rsqrt(lax.optimization_barrier(jnp.mean(values * values, axis=-1, keepdims=True)) + EPS) * gain

def decayed_attention(queries, keys_in, values_in, decay_log_rate):
    length, heads, key_dim = queries.shape
    value_dim = values_in.shape[-1]
    blocks = length // BLOCK

    def to_blocks(array):
        return array.reshape(blocks, BLOCK, heads, array.shape[-1]).transpose(0, 2, 1, 3)
    query_blocks = to_blocks(queries)
    key_blocks = to_blocks(keys_in)
    value_blocks = to_blocks(values_in)
    cumulative = jnp.cumsum(to_blocks(decay_log_rate), axis=2)
    causal = jnp.tril(jnp.ones((BLOCK, BLOCK), dtype=bool))[:, :, None]

    def advance(state, inputs):
        query_blk, key_blk, value_blk, cum_blk = inputs
        relative = cum_blk[:, :, None, :] - cum_blk[:, None, :, :]
        weights = jnp.exp(jnp.where(causal, relative, -jnp.inf))
        scores = jnp.einsum('hid,hjd,hijd->hij', query_blk, key_blk, weights, precision=HIGH)
        inner = jnp.einsum('hij,hjv->hiv', scores, value_blk, precision=HIGH)
        inner = inner + jnp.einsum('hid,hdv->hiv', query_blk * jnp.exp(cum_blk), state, precision=HIGH)
        last = cum_blk[:, -1:, :]
        state = state * jnp.exp(last)[:, 0, :, None] + jnp.einsum('hjd,hjv->hdv', key_blk * jnp.exp(last - cum_blk), value_blk, precision=HIGH)
        return (state, inner)
    initial = jnp.zeros((heads, key_dim, value_dim), jnp.float32)
    _, result = lax.scan(advance, initial, (query_blocks, key_blocks, value_blocks, cumulative))
    return result.transpose(0, 2, 1, 3).reshape(length, heads, value_dim)

def grouped_sum(left, right, groups):
    width = left.shape[1] // groups

    def add_group(index, total):
        start = (index * width).astype(jnp.int32)
        cols = lax.dynamic_slice_in_dim(left, start, width, 1)
        rows = lax.dynamic_slice_in_dim(right, start, width, 0)
        part = jnp.dot(cols, rows, preferred_element_type=jnp.float32)
        rounded = lax.optimization_barrier(part.astype(jnp.bfloat16))
        return total + rounded.astype(jnp.float32)
    empty = jnp.zeros((left.shape[0], right.shape[1]), jnp.float32)
    return lax.fori_loop(jnp.int32(0), jnp.int32(groups), add_group, empty)

def reference(tokens, pre_attention_gain, query_weight, key_weight, value_weight, output_gate_weight, decay_weight, decay_logit_bias, extra_log_decay, head_norm_gain, attention_out_weight, post_attention_gain, pre_feedforward_gain, post_feedforward_gain, up_weight, down_weight):
    stream_in = tokens.astype(jnp.float32)
    normed = root_norm(stream_in, pre_attention_gain).astype(jnp.bfloat16)
    query_rows = jnp.dot(normed, query_weight, preferred_element_type=jnp.float32).astype(jnp.bfloat16)
    key_rows = jnp.dot(normed, key_weight, preferred_element_type=jnp.float32).astype(jnp.bfloat16)
    value_rows = jnp.dot(normed, value_weight, preferred_element_type=jnp.float32).astype(jnp.bfloat16)
    gate_rows = jnp.dot(normed, output_gate_weight, preferred_element_type=jnp.float32).astype(jnp.bfloat16)
    decay_logits = jnp.dot(normed, decay_weight, preferred_element_type=jnp.float32)
    decay_log_rate = jax.nn.log_sigmoid(decay_logits + decay_logit_bias) / GATE_NORM_SCALE + extra_log_decay
    seqs = TOKENS // TOK_DEV
    queries = (query_rows.astype(jnp.float32) * DK ** (-0.5)).reshape(seqs, TOK_DEV, HEADS, DK)
    keys_in = key_rows.astype(jnp.float32).reshape(seqs, TOK_DEV, HEADS, DK)
    values_in = value_rows.astype(jnp.float32).reshape(seqs, TOK_DEV, HEADS, DV)
    decays = decay_log_rate.reshape(seqs, TOK_DEV, HEADS, DK)
    attended = lax.map(lambda item: decayed_attention(*item), (queries, keys_in, values_in, decays))
    attended = attended.reshape(TOKENS, HEADS, DV)
    scaled = attended * lax.rsqrt(lax.optimization_barrier(jnp.mean(attended * attended, axis=-1, keepdims=True)) + EPS)
    scaled = scaled.reshape(TOKENS, V) * head_norm_gain
    headout = (scaled * jax.nn.silu(gate_rows.astype(jnp.float32))).astype(jnp.bfloat16)
    mixed = grouped_sum(headout, attention_out_weight, N_TP)
    stream = stream_in + root_norm(mixed, post_attention_gain)
    normed_mid = root_norm(stream, pre_feedforward_gain).astype(jnp.bfloat16)
    hidden = jnp.square(jax.nn.relu(jnp.dot(normed_mid, up_weight, preferred_element_type=jnp.float32))).astype(jnp.bfloat16)
    feedfwd = grouped_sum(hidden, down_weight, N_TP)
    return (stream + root_norm(feedfwd, post_feedforward_gain)).astype(jnp.bfloat16)
```

```python
import jax
import jax.numpy as jnp
from jax import lax
from jax.sharding import PartitionSpec as P

DK = 64
DV = 128
EPS = 1e-06
GATE_NORM_SCALE = 16.0


def root_norm(rows, gain):
    return rows * lax.rsqrt(jnp.mean(rows * rows, axis=-1, keepdims=True) + EPS) * gain


def split2(x):
    hi = x.astype(jnp.bfloat16)
    lo = (x - hi.astype(jnp.float32)).astype(jnp.bfloat16)
    return hi, lo


def dot_t(a, b):
    return lax.dot_general(a, b, (((1,), (1,)), ((), ())), preferred_element_type=jnp.float32)


def prefix_sums(x):
    length = x.shape[0]
    row = lax.broadcasted_iota(jnp.int32, (length, 1), 0)
    step = 1
    while step < length:
        moved = jnp.concatenate([x[length - step :], x[: length - step]], axis=0)
        x = x + jnp.where(row >= step, moved, 0.0)
        step *= 2
    return x


def attend(q, k, v, log_decay):
    n, width = q.shape
    heads = width // DK
    cum = prefix_sums(log_decay)
    row = lax.broadcasted_iota(jnp.int32, (n, n), 0)
    col = lax.broadcasted_iota(jnp.int32, (n, n), 1)
    lane = lax.broadcasted_iota(jnp.int32, (1, width), 1)

    def per_head(x):
        return jnp.concatenate(
            [jnp.where((lane >= h * DK) & (lane < (h + 1) * DK), x, 0.0) for h in range(heads)], 0
        )

    def scores_of(left, right):
        lh, ll = split2(per_head(left))
        rh, rl = split2(right)
        return dot_t(lh, rh) + dot_t(lh, rl) + dot_t(ll, rh)

    tiled_row = jnp.concatenate([row] * heads, 0)
    tiled_col = jnp.concatenate([col] * heads, 0)
    scores = jnp.where(
        tiled_row == tiled_col,
        dot_t(per_head(q).astype(jnp.bfloat16), k.astype(jnp.bfloat16)),
        0.0,
    )
    half = n // 2
    while half >= 1:
        pieces = []
        for at in range(0, n, 2 * half):
            pieces.append(jnp.broadcast_to(cum[at + half - 1 : at + half], (2 * half, width)))
        bound = jnp.concatenate(pieces, 0) if len(pieces) > 1 else pieces[0]
        fade = jnp.exp(-jnp.abs(cum - bound))
        part = scores_of(q * fade, k * fade)
        keep = (
            (tiled_row // (2 * half) == tiled_col // (2 * half))
            & (tiled_row % (2 * half) >= half)
            & (tiled_col % (2 * half) < half)
        )
        scores = jnp.where(keep, part, scores)
        half //= 2
    outs = []
    for h in range(heads):
        sh, sl = split2(scores[h * n : (h + 1) * n])
        vh = v[:, h * DV : (h + 1) * DV]
        outs.append(
            jnp.dot(sh, vh, preferred_element_type=jnp.float32)
            + jnp.dot(sl, vh, preferred_element_type=jnp.float32)
        )
    return outs


def head_block(acc, bias, extra, gain, qk, v):
    bf = jnp.bfloat16
    q = acc[:, :qk].astype(bf).astype(jnp.float32) * DK ** (-0.5)
    k = acc[:, qk : 2 * qk].astype(bf).astype(jnp.float32)
    x = acc[:, 2 * qk : 3 * qk] + bias
    log_sig = jnp.minimum(x, 0.0) - jnp.log1p(jnp.exp(-jnp.abs(x)))
    rate = log_sig / GATE_NORM_SCALE + extra
    vals = acc[:, 3 * qk : 3 * qk + v].astype(bf)
    gate = acc[:, 3 * qk + v :].astype(bf).astype(jnp.float32)
    outs = attend(q, k, vals, rate)
    scaled = jnp.concatenate(
        [o * lax.rsqrt(jnp.mean(o * o, axis=-1, keepdims=True) + EPS) for o in outs], 1
    )
    return (scaled * gain * (gate / (1.0 + jnp.exp(-gate)))).astype(bf)


def local(
    tokens, pre_attention_gain, query_weight, key_weight, value_weight, output_gate_weight,
    decay_weight, decay_logit_bias, extra_log_decay, head_norm_gain, attention_out_weight,
    post_attention_gain, pre_feedforward_gain, post_feedforward_gain, up_weight, down_weight,
):
    bf = jnp.bfloat16
    n_fs = lax.axis_size("fs")
    n_tp = lax.axis_size("tp")
    length, width = tokens.shape
    share = length // n_tp
    cols = width // n_fs
    qk, v = query_weight.shape[1], value_weight.shape[1]
    stream_in = tokens.astype(jnp.float32)
    normed = root_norm(stream_in, pre_attention_gain).astype(bf)
    joined = jnp.concatenate(
        [query_weight, key_weight, decay_weight, value_weight, output_gate_weight], 1
    )
    whole = lax.all_gather(joined, "fs", axis=0, tiled=True)
    acc = jnp.dot(normed, whole, preferred_element_type=jnp.float32)
    headout = head_block(acc, decay_logit_bias, extra_log_decay, head_norm_gain, qk, v)
    whole_out = lax.all_gather(attention_out_weight, "fs", axis=1, tiled=True)
    mix_part = jnp.dot(headout, whole_out, preferred_element_type=jnp.float32).astype(bf)
    mix = lax.all_to_all(
        mix_part.reshape(n_tp, share, width), "tp", split_axis=0, concat_axis=0, tiled=True
    )
    mixed = jnp.sum(mix.astype(jnp.float32), 0)
    mine = lax.dynamic_slice_in_dim(stream_in, lax.axis_index("tp") * share, share, 0)
    stream = mine + root_norm(mixed, post_attention_gain)
    normed_mid = root_norm(stream, pre_feedforward_gain).astype(bf)
    blocks = normed_mid.reshape(share, n_fs, cols).transpose(1, 0, 2)
    blocks = lax.all_to_all(blocks, "fs", split_axis=0, concat_axis=0, tiled=True)
    rows = lax.all_gather(blocks, "tp", axis=1, tiled=True)
    up = jnp.dot(rows.reshape(n_fs * length, cols), up_weight, preferred_element_type=jnp.float32)
    up = up.astype(bf).reshape(n_fs, length, -1)
    up = lax.all_to_all(up, "fs", split_axis=0, concat_axis=0, tiled=True)
    hidden = jnp.square(jax.nn.relu(jnp.sum(up.astype(jnp.float32), 0))).astype(bf)
    hidden = lax.all_gather(hidden, "fs", axis=0, tiled=True)
    down = jnp.dot(hidden, down_weight, preferred_element_type=jnp.float32).astype(bf)
    down = down.reshape(n_fs, n_tp, share, cols).transpose(1, 0, 2, 3)
    down = lax.all_to_all(down, "tp", split_axis=0, concat_axis=0, tiled=True)
    feed = jnp.sum(down.astype(jnp.float32), 0).astype(bf)
    feed = lax.all_to_all(feed, "fs", split_axis=0, concat_axis=0, tiled=True)
    feed = feed.transpose(1, 0, 2).reshape(share, width).astype(jnp.float32)
    out = (stream + root_norm(feed, post_feedforward_gain)).astype(bf)
    return lax.all_gather(out, "tp", axis=0, tiled=True)


def solution(mesh):
    return jax.shard_map(
        local,
        mesh=mesh,
        in_specs=(
            P(("grp", "fs"), None), P(), P("fs", "tp"), P("fs", "tp"), P("fs", "tp"),
            P("fs", "tp"), P("fs", "tp"), P("tp"), P(("grp", "fs"), "tp"), P("tp"),
            P("tp", "fs"), P(), P(), P(), P("fs", "tp"), P("tp", "fs"),
        ),
        out_specs=P(("grp", "fs"), None),
        check_vma=False,
    )
```

```python
import jax
import jax.numpy as jnp
from jax import lax
from jax.experimental import pallas as pl
from jax.experimental.pallas import tpu as pltpu
from jax.sharding import PartitionSpec as P

DK = 64
DV = 128
EPS = 1e-06
GATE_NORM_SCALE = 16.0


def root_norm(rows, gain):
    return rows * lax.rsqrt(jnp.mean(rows * rows, axis=-1, keepdims=True) + EPS) * gain


def split2(x):
    hi = x.astype(jnp.bfloat16)
    lo = (x - hi.astype(jnp.float32)).astype(jnp.bfloat16)
    return hi, lo


def dot_t(a, b):
    return lax.dot_general(a, b, (((1,), (1,)), ((), ())), preferred_element_type=jnp.float32)


def split3(x):
    hi = x.astype(jnp.bfloat16)
    rest = x - hi.astype(jnp.float32)
    mid = rest.astype(jnp.bfloat16)
    return hi, mid, (rest - mid.astype(jnp.float32)).astype(jnp.bfloat16)


def pick(mask, parts):
    chosen = mask.astype(jnp.float32).astype(jnp.bfloat16)
    total = 0.0
    for part in parts:
        total = total + jnp.dot(chosen, part, preferred_element_type=jnp.float32)
    return total


def attend(q, k, v, log_decay):
    n, width = q.shape
    heads = width // DK
    row = lax.broadcasted_iota(jnp.int32, (n, n), 0)
    col = lax.broadcasted_iota(jnp.int32, (n, n), 1)
    lane = lax.broadcasted_iota(jnp.int32, (n, width), 1)
    cum = pick(row >= col, split3(log_decay))
    cum_parts = split3(cum)

    def per_head(x):
        return jnp.concatenate(
            [jnp.where((lane >= h * DK) & (lane < (h + 1) * DK), x, 0.0) for h in range(heads)], 0
        )

    def scores_of(left, right):
        lh, ll = split2(per_head(left))
        rh, rl = split2(right)
        return dot_t(lh, rh) + dot_t(lh, rl) + dot_t(ll, rh)

    tiled_row = jnp.concatenate([row] * heads, 0)
    tiled_col = jnp.concatenate([col] * heads, 0)
    scores = jnp.where(
        tiled_row == tiled_col,
        dot_t(per_head(q).astype(jnp.bfloat16), k.astype(jnp.bfloat16)),
        0.0,
    )
    half = n // 2
    while half >= 1:
        bound = pick(col == (row & ~(2 * half - 1)) + (half - 1), cum_parts)
        fade = jnp.exp(-jnp.abs(cum - bound))
        part = scores_of(q * fade, k * fade)
        apart = tiled_row ^ tiled_col
        keep = (apart >= half) & (apart < 2 * half) & (tiled_row > tiled_col)
        scores = jnp.where(keep, part, scores)
        half //= 2
    outs = []
    for h in range(heads):
        sh, sl = split2(scores[h * n : (h + 1) * n])
        vh = v[:, h * DV : (h + 1) * DV]
        outs.append(
            jnp.dot(sh, vh, preferred_element_type=jnp.float32)
            + jnp.dot(sl, vh, preferred_element_type=jnp.float32)
        )
    return outs


def head_block(acc, bias, extra, gain, qk, v):
    bf = jnp.bfloat16
    q = acc[:, :qk].astype(bf).astype(jnp.float32) * DK ** (-0.5)
    k = acc[:, qk : 2 * qk].astype(bf).astype(jnp.float32)
    x = acc[:, 2 * qk : 3 * qk] + bias
    log_sig = jnp.minimum(x, 0.0) - jnp.log1p(jnp.exp(-jnp.abs(x)))
    rate = log_sig / GATE_NORM_SCALE + extra
    vals = acc[:, 3 * qk : 3 * qk + v].astype(bf)
    gate = acc[:, 3 * qk + v :].astype(bf).astype(jnp.float32)
    outs = attend(q, k, vals, rate)
    scaled = jnp.concatenate(
        [o * lax.rsqrt(jnp.mean(o * o, axis=-1, keepdims=True) + EPS) for o in outs], 1
    )
    return (scaled * gain * (gate / (1.0 + jnp.exp(-gate)))).astype(bf)


def local_plain(
    tokens, pre_attention_gain, query_weight, key_weight, value_weight, output_gate_weight,
    decay_weight, decay_logit_bias, extra_log_decay, head_norm_gain, attention_out_weight,
    post_attention_gain, pre_feedforward_gain, post_feedforward_gain, up_weight, down_weight,
):
    bf = jnp.bfloat16
    n_fs = lax.axis_size("fs")
    n_tp = lax.axis_size("tp")
    length, width = tokens.shape
    share = length // n_tp
    cols = width // n_fs
    qk, v = query_weight.shape[1], value_weight.shape[1]
    stream_in = tokens.astype(jnp.float32)
    normed = root_norm(stream_in, pre_attention_gain).astype(bf)
    joined = jnp.concatenate(
        [query_weight, key_weight, decay_weight, value_weight, output_gate_weight], 1
    )
    whole = lax.all_gather(joined, "fs", axis=0, tiled=True)
    acc = jnp.dot(normed, whole, preferred_element_type=jnp.float32)
    headout = head_block(acc, decay_logit_bias, extra_log_decay, head_norm_gain, qk, v)
    whole_out = lax.all_gather(attention_out_weight, "fs", axis=1, tiled=True)
    mix_part = jnp.dot(headout, whole_out, preferred_element_type=jnp.float32).astype(bf)
    mix = lax.all_to_all(
        mix_part.reshape(n_tp, share, width), "tp", split_axis=0, concat_axis=0, tiled=True
    )
    mixed = jnp.sum(mix.astype(jnp.float32), 0)
    mine = lax.dynamic_slice_in_dim(stream_in, lax.axis_index("tp") * share, share, 0)
    stream = mine + root_norm(mixed, post_attention_gain)
    normed_mid = root_norm(stream, pre_feedforward_gain).astype(bf)
    blocks = normed_mid.reshape(share, n_fs, cols).transpose(1, 0, 2)
    blocks = lax.all_to_all(blocks, "fs", split_axis=0, concat_axis=0, tiled=True)
    rows = lax.all_gather(blocks, "tp", axis=1, tiled=True)
    up = jnp.dot(rows.reshape(n_fs * length, cols), up_weight, preferred_element_type=jnp.float32)
    up = up.astype(bf).reshape(n_fs, length, -1)
    up = lax.all_to_all(up, "fs", split_axis=0, concat_axis=0, tiled=True)
    hidden = jnp.square(jax.nn.relu(jnp.sum(up.astype(jnp.float32), 0))).astype(bf)
    hidden = lax.all_gather(hidden, "fs", axis=0, tiled=True)
    down = jnp.dot(hidden, down_weight, preferred_element_type=jnp.float32).astype(bf)
    down = down.reshape(n_fs, n_tp, share, cols).transpose(1, 0, 2, 3)
    down = lax.all_to_all(down, "tp", split_axis=0, concat_axis=0, tiled=True)
    feed = jnp.sum(down.astype(jnp.float32), 0).astype(bf)
    feed = lax.all_to_all(feed, "fs", split_axis=0, concat_axis=0, tiled=True)
    feed = feed.transpose(1, 0, 2).reshape(share, width).astype(jnp.float32)
    out = (stream + root_norm(feed, post_feedforward_gain)).astype(bf)
    return lax.all_gather(out, "tp", axis=0, tiled=True)


def exchange_kernel(
    x_ref, join_ref, bias_ref, extra_ref, head_gain_ref, wo_ref, gain_a_ref, gain_b_ref,
    gain_c_ref, gain_d_ref, up_ref, down_ref, out_ref,
    nm, no, jp, p32s, p16s, p32r, p16r, wop, mixs, mixr, st, mid, mo, mx,
    upp, dnp, us, ur, hs, hr, ds, fr, own_up, send, recv, *, n_fs, n_tp, qk, v,
):
    bf, f32 = jnp.bfloat16, jnp.float32
    g, f, t = lax.axis_index("grp"), lax.axis_index("fs"), lax.axis_index("tp")
    pair, far, b, half = f ^ 1, f ^ 2, f & 1, f >> 1
    share = out_ref.shape[1]
    cols = mid.shape[2]
    length = n_tp * share
    waiting = []
    count = [0]

    def slots(n):
        first = count[0]
        count[0] += n
        return first

    def put(src, dst, at, **where):
        copy = pltpu.make_async_remote_copy(
            src_ref=src, dst_ref=dst, send_sem=send.at[at], recv_sem=recv.at[at],
            device_id=where, device_id_type=pl.DeviceIdType.MESH,
        )
        copy.start()
        waiting.append(copy)

    def take(dst, at):
        pltpu.make_async_remote_copy(
            src_ref=dst, dst_ref=dst, send_sem=send.at[at], recv_sem=recv.at[at],
            device_id={"fs": far}, device_id_type=pl.DeviceIdType.MESH,
        ).wait_recv()

    barrier = pltpu.get_barrier_semaphore()
    peers = [{"grp": 1 - g}]
    peers += [{"fs": f ^ s} for s in range(1, n_fs)]
    peers += [{"tp": t ^ k} for k in range(1, n_tp)]
    peers += [{"fs": far, "tp": t ^ k} for k in range(1, n_tp)]
    for peer in peers:
        pl.semaphore_signal(barrier, inc=1, device_id=peer, device_id_type=pl.DeviceIdType.MESH)
    pl.semaphore_wait(barrier, len(peers))

    def piece(ref, part, i, pieces):
        size = ref.shape[0] // (2 * pieces)
        at = pl.multiple_of(part * (pieces * size) + i * size, size)
        return ref.at[pl.ds(at, size)]

    def fetch(ref, into, pieces):
        at = slots(2 * pieces)
        for i in range(pieces):
            put(piece(ref, g, i, pieces), piece(into, g, i, pieces), at + i, fs=pair)
        return at

    def pass_on(into, at, pieces):
        for i in range(pieces):
            take(piece(into, g, i, pieces), at + i)
            put(piece(into, g, i, pieces), piece(into, g, i, pieces), at + pieces + i, grp=1 - g)

    def settle(into, at, pieces):
        for i in range(pieces):
            take(piece(into, 1 - g, i, pieces), at + pieces + i)

    join_at = fetch(join_ref, jp, 2)

    def squares(blocks):
        total = 0.0
        for block in blocks:
            total = total + jnp.sum(block * block, axis=-1, keepdims=True)
        return lax.rsqrt(total / (n_fs * cols) + EPS)

    x = [x_ref[:, :, c * cols : (c + 1) * cols].reshape(length, cols).astype(f32) for c in range(n_fs)]
    scale = squares(x)
    for c in range(n_fs):
        nm[c] = (x[c] * scale * gain_a_ref[c]).astype(bf)
    no_at = slots(1)
    put(nm.at[pl.ds(2 * (1 - half), 2)], no, no_at, fs=far)

    wo_at = slots(2 * n_fs)
    rows_wo = wo_ref.shape[0] // 2

    def wo_part(ref, part):
        return ref.at[pl.ds(pl.multiple_of(part * rows_wo, rows_wo), rows_wo)]

    for s in (2, 3, 1):
        put(wo_part(wo_ref, g), wo_part(wop.at[f], g), wo_at + s, fs=f ^ s)

    up_at = fetch(up_ref, upp, 2)
    down_at = fetch(down_ref, dnp, 2)
    pass_on(jp, join_at, 2)
    take(no, no_at)
    settle(jp, join_at, 2)

    def dot(l, r):
        return jnp.dot(l, r, preferred_element_type=f32)

    part_at = slots(2)
    other = dot(no[b], join_ref[...]) + dot(no[1 - b], jp[...])
    p32s[...] = other[:, : 3 * qk]
    put(p32s, p32r, part_at, fs=far)
    p16s[...] = other[:, 3 * qk :].astype(bf)
    put(p16s, p16r, part_at + 1, fs=far)
    acc = dot(nm[f], join_ref[...]) + dot(nm[pair], jp[...])
    for s in (1, 2, 3):
        take(wo_part(wop.at[f ^ s], g), wo_at + s)
        put(wo_part(wop.at[f ^ s], g), wo_part(wop.at[f ^ s], g), wo_at + n_fs + s, grp=1 - g)
    take(p32r, part_at)
    take(p16r, part_at + 1)
    acc = jnp.concatenate([acc[:, : 3 * qk] + p32r[...], acc[:, 3 * qk :] + p16r[...].astype(f32)], 1)
    headout = head_block(acc, bias_ref[...], extra_ref[...], head_gain_ref[...], qk, v)
    for s in (1, 2, 3):
        take(wo_part(wop.at[f ^ s], 1 - g), wo_at + n_fs + s)
    for s in range(n_fs):
        weight = wo_ref[...] if s == 0 else wop[f ^ s]
        block = dot(headout, weight).astype(bf)
        for k in range(n_tp):
            mixs[k, f ^ s] = block[k * share : (k + 1) * share]
    mix_at = slots(n_tp)
    for k in range(1, n_tp):
        put(mixs.at[t ^ k], mixr.at[t], mix_at + k, tp=t ^ k)
    pass_on(upp, up_at, 2)
    mix = mixs[t].astype(f32)
    for k in range(1, n_tp):
        take(mixr.at[t ^ k], mix_at + k)
        mix = mix + mixr[t ^ k].astype(f32)
    mix = [mix[c] for c in range(n_fs)]
    scale = squares(mix)
    mine = [x_ref[t, :, c * cols : (c + 1) * cols].astype(f32) for c in range(n_fs)]
    stream = [mine[c] + mix[c] * scale * gain_b_ref[c] for c in range(n_fs)]
    scale = squares(stream)
    for c in range(n_fs):
        st[c] = stream[c]
        mid[c] = (stream[c] * scale * gain_c_ref[c]).astype(bf)
    mx_at, mo_at = slots(n_tp), slots(n_tp)
    for k in range(n_tp):
        put(mid.at[pl.ds(2 * (1 - half), 2)], mx.at[t], mx_at + k, fs=far, tp=t ^ k)
    for k in range(1, n_tp):
        put(mid.at[pl.ds(2 * half, 2)], mo.at[t], mo_at + k, tp=t ^ k)
    mo[t, 0] = mid[2 * half]
    mo[t, 1] = mid[2 * half + 1]
    settle(upp, up_at, 2)
    for k in range(n_tp):
        take(mx.at[t ^ k], mx_at + k)

    chunks = us.shape[0]
    wide = us.shape[2]

    def rows_of(ref, at):
        return ref[:, at].reshape(length, cols)

    us_at = slots(chunks)
    far_own, far_pair = rows_of(mx, b), rows_of(mx, 1 - b)
    for c in range(chunks):
        at = slice(c * wide, (c + 1) * wide)
        us[c] = (dot(far_own, up_ref[:, at]) + dot(far_pair, upp[:, at])).astype(bf)
        put(us.at[c], ur.at[c], us_at + c, fs=far)
    for k in range(1, n_tp):
        take(mo.at[t ^ k], mo_at + k)
    near_own, near_pair = rows_of(mo, b), rows_of(mo, 1 - b)
    for c in range(chunks):
        at = slice(c * wide, (c + 1) * wide)
        own_up[c] = dot(near_own, up_ref[:, at]) + dot(near_pair, upp[:, at])
    hs_at = slots(chunks)
    for c in range(chunks):
        take(ur.at[c], us_at + c)
        hidden = jnp.maximum(own_up[c] + ur[c].astype(f32), 0.0)
        hs[c] = (hidden * hidden).astype(bf)
        put(hs.at[c], hr.at[c], hs_at + c, fs=far)
    pass_on(dnp, down_at, 2)
    settle(dnp, down_at, 2)

    def project(ref, into, ready):
        first = second = 0.0
        for c in range(chunks):
            if ready is not None:
                take(ref.at[c], ready + c)
            at = slice(c * wide, (c + 1) * wide)
            first = first + dot(ref[c], down_ref[at])
            second = second + dot(ref[c], dnp[at])
        first, second = first.astype(bf), second.astype(bf)
        for k in range(n_tp):
            into[k, b] = first[k * share : (k + 1) * share]
            into[k, 1 - b] = second[k * share : (k + 1) * share]

    near_at, far_at = slots(n_tp), slots(n_tp)
    project(hs, ds.at[0], None)
    for k in range(1, n_tp):
        put(ds.at[0, t ^ k], fr.at[t, half], near_at + k, tp=t ^ k)
    fr[t, half] = ds[0, t]
    project(hr, ds.at[1], hs_at)
    for k in range(n_tp):
        put(ds.at[1, t ^ k], fr.at[t, half], far_at + k, fs=far, tp=t ^ k)
    for k in range(1, n_tp):
        take(fr.at[t ^ k, half], near_at + k)
    for k in range(n_tp):
        take(fr.at[t ^ k, 1 - half], far_at + k)
    feed = []
    for c in range(n_fs):
        total = 0.0
        for k in range(n_tp):
            total = total + fr[k, c // 2, c % 2].astype(f32)
        feed.append(total)
    scale = squares(feed)
    for c in range(n_fs):
        out_ref[t, :, c * cols : (c + 1) * cols] = (
            st[c] + feed[c] * scale * gain_d_ref[c]
        ).astype(bf)
    out_at = slots(n_tp)
    for k in range(1, n_tp):
        put(out_ref.at[t], out_ref.at[t], out_at + k, tp=t ^ k)
    for k in range(1, n_tp):
        take(out_ref.at[t ^ k], out_at + k)
    for copy in waiting:
        copy.wait_send()
    assert count[0] <= send.shape[0]


def local_fused(
    tokens, pre_attention_gain, query_weight, key_weight, value_weight, output_gate_weight,
    decay_weight, decay_logit_bias, extra_log_decay, head_norm_gain, attention_out_weight,
    post_attention_gain, pre_feedforward_gain, post_feedforward_gain, up_weight, down_weight,
):
    bf, f32 = jnp.bfloat16, jnp.float32
    n_fs, n_tp = lax.axis_size("fs"), lax.axis_size("tp")
    length, width = tokens.shape
    share, cols = length // n_tp, width // n_fs
    qk, v = query_weight.shape[1], value_weight.shape[1]
    units = up_weight.shape[1]
    chunks = 4
    joined = jnp.concatenate(
        [query_weight, key_weight, decay_weight, value_weight, output_gate_weight], 1
    )
    total = joined.shape[1]
    vm = pltpu.VMEM
    block = (n_fs, share, cols)
    scratch = [
        vm((n_fs, length, cols), bf), vm((2, length, cols), bf), vm(joined.shape, bf),
        vm((length, 3 * qk), f32), vm((length, 2 * v), bf),
        vm((length, 3 * qk), f32), vm((length, 2 * v), bf),
        vm((n_fs,) + attention_out_weight.shape, bf),
        vm((n_tp,) + block, bf), vm((n_tp,) + block, bf), vm(block, f32), vm(block, bf),
        vm((n_tp, 2, share, cols), bf), vm((n_tp, 2, share, cols), bf),
        vm(up_weight.shape, bf), vm(down_weight.shape, bf),
        vm((chunks, length, units // chunks), bf), vm((chunks, length, units // chunks), bf),
        vm((chunks, length, units // chunks), bf), vm((chunks, length, units // chunks), bf),
        vm((2, n_tp, 2, share, cols), bf), vm((n_tp, 2, 2, share, cols), bf),
        vm((chunks, length, units // chunks), f32),
        pltpu.SemaphoreType.DMA((64,)), pltpu.SemaphoreType.DMA((64,)),
    ]

    def kernel(*refs):
        exchange_kernel(*refs, n_fs=n_fs, n_tp=n_tp, qk=qk, v=v)

    def gain_blocks(gain):
        return gain.reshape(n_fs, 1, cols)

    out = pl.pallas_call(
        kernel,
        out_shape=jax.ShapeDtypeStruct((n_tp, share, width), bf),
        in_specs=[pl.BlockSpec(memory_space=pltpu.VMEM)] * 12,
        out_specs=pl.BlockSpec(memory_space=pltpu.VMEM),
        scratch_shapes=scratch,
        compiler_params=pltpu.CompilerParams(
            collective_id=0, has_side_effects=True, vmem_limit_bytes=60 * 2**20
        ),
    )(
        tokens.reshape(n_tp, share, width), joined, decay_logit_bias.reshape(1, qk),
        extra_log_decay, head_norm_gain.reshape(1, v), attention_out_weight,
        gain_blocks(pre_attention_gain), gain_blocks(post_attention_gain),
        gain_blocks(pre_feedforward_gain), gain_blocks(post_feedforward_gain),
        up_weight, down_weight,
    )
    return out.reshape(length, width)


def local(*arrays):
    n_fs, n_tp, n_grp = (lax.axis_size(name) for name in ("fs", "tp", "grp"))
    length, width = arrays[0].shape
    fits = n_fs == 4 and n_grp == 2 and n_tp in (2, 4, 8) and width // n_fs % 128 == 0
    fits = fits and length % (n_tp * 16) == 0 and arrays[2].shape[1] % 128 == 0
    fits = fits and arrays[-2].shape[1] % 512 == 0
    return local_fused(*arrays) if fits else local_plain(*arrays)


def solution(mesh):
    return jax.shard_map(
        local,
        mesh=mesh,
        in_specs=(
            P(("grp", "fs"), None), P(), P("fs", "tp"), P("fs", "tp"), P("fs", "tp"),
            P("fs", "tp"), P("fs", "tp"), P("tp"), P(("grp", "fs"), "tp"), P("tp"),
            P("tp", "fs"), P(), P(), P(), P("fs", "tp"), P("tp", "fs"),
        ),
        out_specs=P(("grp", "fs"), None),
        check_vma=False,
    )
```

```python
import jax
import jax.numpy as jnp
from jax import lax
from jax.experimental import pallas as pl
from jax.experimental.pallas import tpu as pltpu
from jax.sharding import PartitionSpec as P

DK = 64
DV = 128
EPS = 1e-06
GATE_NORM_SCALE = 16.0


def root_norm(rows, gain):
    return rows * lax.rsqrt(jnp.mean(rows * rows, axis=-1, keepdims=True) + EPS) * gain


def split2(x):
    hi = x.astype(jnp.bfloat16)
    lo = (x - hi.astype(jnp.float32)).astype(jnp.bfloat16)
    return hi, lo


def dot_t(a, b):
    return lax.dot_general(a, b, (((1,), (1,)), ((), ())), preferred_element_type=jnp.float32)


def split3(x):
    hi = x.astype(jnp.bfloat16)
    rest = x - hi.astype(jnp.float32)
    mid = rest.astype(jnp.bfloat16)
    return hi, mid, (rest - mid.astype(jnp.float32)).astype(jnp.bfloat16)


def pick(mask, parts):
    chosen = mask.astype(jnp.float32).astype(jnp.bfloat16)
    total = 0.0
    for part in parts:
        total = total + jnp.dot(chosen, part, preferred_element_type=jnp.float32)
    return total


def attend(q, k, v, log_decay):
    n, width = q.shape
    heads = width // DK
    row = lax.broadcasted_iota(jnp.int32, (n, n), 0)
    col = lax.broadcasted_iota(jnp.int32, (n, n), 1)
    lane = lax.broadcasted_iota(jnp.int32, (n, width), 1)
    cum = pick(row >= col, split3(log_decay))
    cum_parts = split3(cum)

    def per_head(x):
        return jnp.concatenate(
            [jnp.where((lane >= h * DK) & (lane < (h + 1) * DK), x, 0.0) for h in range(heads)], 0
        )

    def scores_of(left, right):
        lh, ll = split2(per_head(left))
        rh, rl = split2(right)
        return dot_t(lh, rh) + dot_t(lh, rl) + dot_t(ll, rh)

    tiled_row = jnp.concatenate([row] * heads, 0)
    tiled_col = jnp.concatenate([col] * heads, 0)
    scores = jnp.where(
        tiled_row == tiled_col,
        dot_t(per_head(q).astype(jnp.bfloat16), k.astype(jnp.bfloat16)),
        0.0,
    )
    half = n // 2
    while half >= 1:
        bound = pick(col == (row & ~(2 * half - 1)) + (half - 1), cum_parts)
        fade = jnp.exp(-jnp.abs(cum - bound))
        part = scores_of(q * fade, k * fade)
        apart = tiled_row ^ tiled_col
        keep = (apart >= half) & (apart < 2 * half) & (tiled_row > tiled_col)
        scores = jnp.where(keep, part, scores)
        half //= 2
    outs = []
    for h in range(heads):
        sh, sl = split2(scores[h * n : (h + 1) * n])
        vh = v[:, h * DV : (h + 1) * DV]
        outs.append(
            jnp.dot(sh, vh, preferred_element_type=jnp.float32)
            + jnp.dot(sl, vh, preferred_element_type=jnp.float32)
        )
    return outs


def head_block(acc, bias, extra, gain, qk, v):
    bf = jnp.bfloat16
    q = acc[:, :qk].astype(bf).astype(jnp.float32) * DK ** (-0.5)
    k = acc[:, qk : 2 * qk].astype(bf).astype(jnp.float32)
    x = acc[:, 2 * qk : 3 * qk] + bias
    log_sig = jnp.minimum(x, 0.0) - jnp.log1p(jnp.exp(-jnp.abs(x)))
    rate = log_sig / GATE_NORM_SCALE + extra
    vals = acc[:, 3 * qk : 3 * qk + v].astype(bf)
    gate = acc[:, 3 * qk + v :].astype(bf).astype(jnp.float32)
    outs = attend(q, k, vals, rate)
    scaled = jnp.concatenate(
        [o * lax.rsqrt(jnp.mean(o * o, axis=-1, keepdims=True) + EPS) for o in outs], 1
    )
    return (scaled * gain * (gate / (1.0 + jnp.exp(-gate)))).astype(bf)


def local_plain(
    tokens, pre_attention_gain, query_weight, key_weight, value_weight, output_gate_weight,
    decay_weight, decay_logit_bias, extra_log_decay, head_norm_gain, attention_out_weight,
    post_attention_gain, pre_feedforward_gain, post_feedforward_gain, up_weight, down_weight,
):
    bf = jnp.bfloat16
    n_fs = lax.axis_size("fs")
    n_tp = lax.axis_size("tp")
    length, width = tokens.shape
    share = length // n_tp
    cols = width // n_fs
    qk, v = query_weight.shape[1], value_weight.shape[1]
    stream_in = tokens.astype(jnp.float32)
    normed = root_norm(stream_in, pre_attention_gain).astype(bf)
    joined = jnp.concatenate(
        [query_weight, key_weight, decay_weight, value_weight, output_gate_weight], 1
    )
    whole = lax.all_gather(joined, "fs", axis=0, tiled=True)
    acc = jnp.dot(normed, whole, preferred_element_type=jnp.float32)
    headout = head_block(acc, decay_logit_bias, extra_log_decay, head_norm_gain, qk, v)
    whole_out = lax.all_gather(attention_out_weight, "fs", axis=1, tiled=True)
    mix_part = jnp.dot(headout, whole_out, preferred_element_type=jnp.float32).astype(bf)
    mix = lax.all_to_all(
        mix_part.reshape(n_tp, share, width), "tp", split_axis=0, concat_axis=0, tiled=True
    )
    mixed = jnp.sum(mix.astype(jnp.float32), 0)
    mine = lax.dynamic_slice_in_dim(stream_in, lax.axis_index("tp") * share, share, 0)
    stream = mine + root_norm(mixed, post_attention_gain)
    normed_mid = root_norm(stream, pre_feedforward_gain).astype(bf)
    blocks = normed_mid.reshape(share, n_fs, cols).transpose(1, 0, 2)
    blocks = lax.all_to_all(blocks, "fs", split_axis=0, concat_axis=0, tiled=True)
    rows = lax.all_gather(blocks, "tp", axis=1, tiled=True)
    up = jnp.dot(rows.reshape(n_fs * length, cols), up_weight, preferred_element_type=jnp.float32)
    up = up.astype(bf).reshape(n_fs, length, -1)
    up = lax.all_to_all(up, "fs", split_axis=0, concat_axis=0, tiled=True)
    hidden = jnp.square(jax.nn.relu(jnp.sum(up.astype(jnp.float32), 0))).astype(bf)
    hidden = lax.all_gather(hidden, "fs", axis=0, tiled=True)
    down = jnp.dot(hidden, down_weight, preferred_element_type=jnp.float32).astype(bf)
    down = down.reshape(n_fs, n_tp, share, cols).transpose(1, 0, 2, 3)
    down = lax.all_to_all(down, "tp", split_axis=0, concat_axis=0, tiled=True)
    feed = jnp.sum(down.astype(jnp.float32), 0).astype(bf)
    feed = lax.all_to_all(feed, "fs", split_axis=0, concat_axis=0, tiled=True)
    feed = feed.transpose(1, 0, 2).reshape(share, width).astype(jnp.float32)
    out = (stream + root_norm(feed, post_feedforward_gain)).astype(bf)
    return lax.all_gather(out, "tp", axis=0, tiled=True)


def exchange_kernel(
    x_ref, q_ref, k_ref, d_ref, v_ref, g_ref, bias_ref, extra_ref, head_gain_ref, wo_ref,
    gain_a_ref, gain_b_ref, gain_c_ref, gain_d_ref, up_ref, down_ref, out_ref,
    nm, no, qp, kp, dp, vp, gp, p32s, p16s, p32r, p16r, wop, mixs, mixr, st, mid, mo, mx,
    upp, dnp, us, ur, hs, hr, ds, fr, fq, fs_, fz, ff, own_up, send, recv,
    *, n_fs, n_tp, qk, v,
):
    bf, f32 = jnp.bfloat16, jnp.float32
    g, f, t = lax.axis_index("grp"), lax.axis_index("fs"), lax.axis_index("tp")
    pair, far, b, half = f ^ 1, f ^ 2, f & 1, f >> 1
    share = out_ref.shape[1]
    cols = mid.shape[2]
    length = n_tp * share
    waiting = []
    count = [0]

    def slots(n):
        first = count[0]
        count[0] += n
        return first

    def put(src, dst, at, **where):
        copy = pltpu.make_async_remote_copy(
            src_ref=src, dst_ref=dst, send_sem=send.at[at], recv_sem=recv.at[at],
            device_id=where, device_id_type=pl.DeviceIdType.MESH,
        )
        copy.start()
        waiting.append(copy)

    def take(dst, at):
        pltpu.make_async_remote_copy(
            src_ref=dst, dst_ref=dst, send_sem=send.at[at], recv_sem=recv.at[at],
            device_id={"fs": far}, device_id_type=pl.DeviceIdType.MESH,
        ).wait_recv()

    barrier = pltpu.get_barrier_semaphore()
    peers = [{"grp": 1 - g}]
    peers += [{"fs": f ^ s} for s in range(1, n_fs)]
    peers += [{"tp": t ^ k} for k in range(1, n_tp)]
    for peer in peers:
        pl.semaphore_signal(barrier, inc=1, device_id=peer, device_id_type=pl.DeviceIdType.MESH)
    pl.semaphore_wait(barrier, len(peers))

    class Fetch:
        def __init__(self, ref, into, pieces):
            self.ref, self.into, self.pieces = ref, into, pieces
            self.at = slots(2 * pieces)
            self.size = ref.shape[0] // (2 * pieces)

        def piece(self, ref, part, i):
            at = pl.multiple_of(part * (self.pieces * self.size) + i * self.size, self.size)
            return ref.at[pl.ds(at, self.size)]

        def start(self, i):
            put(self.piece(self.ref, g, i), self.piece(self.into, g, i), self.at + i, fs=pair)

        def pass_on(self, i):
            mine = self.piece(self.into, g, i)
            take(mine, self.at + i)
            put(mine, mine, self.at + self.pieces + i, grp=1 - g)

        def settle(self):
            for i in range(self.pieces):
                take(self.piece(self.into, 1 - g, i), self.at + self.pieces + i)

    def gather_rows(ref, at):
        for k in range(1, n_tp):
            put(ref.at[t], ref.at[t], at + k, tp=t ^ k)

    def take_rows(ref, at):
        for k in range(1, n_tp):
            take(ref.at[t ^ k], at + k)

    def rows_of(ref, at):
        return ref[:, at].reshape(length, cols)

    def dot(l, r):
        return jnp.dot(l, r, preferred_element_type=f32)

    def squares(blocks):
        total = 0.0
        for block in blocks:
            total = total + jnp.sum(block * block, axis=-1, keepdims=True)
        return lax.rsqrt(total / (n_fs * cols) + EPS)

    projections = [Fetch(r, p, 1) for r, p in zip((q_ref, k_ref, d_ref, v_ref, g_ref), (qp, kp, dp, vp, gp))]
    for weight in projections:
        weight.start(0)

    x = [x_ref[:, :, c * cols : (c + 1) * cols].astype(f32) for c in range(n_fs)]
    scale = squares(x)
    for c in range(n_fs):
        nm[:, c] = (x[c] * scale * gain_a_ref[c]).astype(bf)
    no_at = slots(n_tp)
    put(nm.at[t, pl.ds(2 * (1 - half), 2)], no.at[t], no_at, fs=far)

    wo_at = slots(2 * n_fs)
    rows_wo = wo_ref.shape[0] // 2

    def wo_part(ref, part):
        return ref.at[pl.ds(pl.multiple_of(part * rows_wo, rows_wo), rows_wo)]

    for s in (2, 3, 1):
        put(wo_part(wo_ref, g), wo_part(wop.at[f], g), wo_at + s, fs=f ^ s)

    projections[0].pass_on(0)
    projections[1].pass_on(0)
    take(no.at[t], no_at)
    gather_rows(no, no_at)
    for weight in projections[2:]:
        weight.pass_on(0)
    take_rows(no, no_at)

    up = Fetch(up_ref, upp, 4)
    down = Fetch(down_ref, dnp, 8)
    part_at = slots(5)
    no_own, no_pair = rows_of(no, b), rows_of(no, 1 - b)
    outgoing = [p32s.at[0], p32s.at[1], p32s.at[2], p16s.at[0], p16s.at[1]]
    incoming = [p32r.at[0], p32r.at[1], p32r.at[2], p16r.at[0], p16r.at[1]]
    for i, weight in enumerate(projections):
        weight.settle()
        other = dot(no_own, weight.ref[...]) + dot(no_pair, weight.into[...])
        outgoing[i][...] = other.astype(outgoing[i].dtype)
        put(outgoing[i], incoming[i], part_at + i, fs=far)
    for i in range(4):
        up.start(i)
    nm_own, nm_pair = rows_of(nm, f), rows_of(nm, pair)
    acc = [dot(nm_own, w.ref[...]) + dot(nm_pair, w.into[...]) for w in projections]
    for s in (1, 2, 3):
        mine = wo_part(wop.at[f ^ s], g)
        take(mine, wo_at + s)
        put(mine, mine, wo_at + n_fs + s, grp=1 - g)
    for i in range(5):
        take(incoming[i], part_at + i)
        acc[i] = acc[i] + incoming[i][...].astype(f32)
    headout = head_block(
        jnp.concatenate(acc, 1), bias_ref[...], extra_ref[...], head_gain_ref[...], qk, v
    )
    for s in (1, 2, 3):
        take(wo_part(wop.at[f ^ s], 1 - g), wo_at + n_fs + s)
    for s in range(n_fs):
        weight = wo_ref[...] if s == 0 else wop[f ^ s]
        block = dot(headout, weight).astype(bf)
        for k in range(n_tp):
            mixs[k, f ^ s] = block[k * share : (k + 1) * share]
    mix_at = slots(n_tp)
    for k in range(1, n_tp):
        put(mixs.at[t ^ k], mixr.at[t], mix_at + k, tp=t ^ k)
    up.pass_on(0)
    up.pass_on(1)
    mix = mixs[t].astype(f32)
    for k in range(1, n_tp):
        take(mixr.at[t ^ k], mix_at + k)
        mix = mix + mixr[t ^ k].astype(f32)
    mix = [mix[c] for c in range(n_fs)]
    scale = squares(mix)
    mine = [x_ref[t, :, c * cols : (c + 1) * cols].astype(f32) for c in range(n_fs)]
    stream = [mine[c] + mix[c] * scale * gain_b_ref[c] for c in range(n_fs)]
    scale = squares(stream)
    for c in range(n_fs):
        st[c] = stream[c]
        mid[c] = (stream[c] * scale * gain_c_ref[c]).astype(bf)
    mx_at, mo_at = slots(n_tp), slots(n_tp)
    put(mid.at[pl.ds(2 * (1 - half), 2)], mx.at[t], mx_at, fs=far)
    for k in range(1, n_tp):
        put(mid.at[pl.ds(2 * half, 2)], mo.at[t], mo_at + k, tp=t ^ k)
    down.start(0)
    down.start(1)
    mo[t, 0] = mid[2 * half]
    mo[t, 1] = mid[2 * half + 1]
    take(mx.at[t], mx_at)
    gather_rows(mx, mx_at)
    up.pass_on(2)
    up.pass_on(3)
    take_rows(mx, mx_at)
    up.settle()

    chunks = us.shape[0]
    wide = us.shape[2]
    us_at = slots(chunks)
    far_own, far_pair = rows_of(mx, b), rows_of(mx, 1 - b)
    for c in range(chunks):
        at = slice(c * wide, (c + 1) * wide)
        us[c] = (dot(far_own, up_ref[:, at]) + dot(far_pair, upp[:, at])).astype(bf)
        put(us.at[c], ur.at[c], us_at + c, fs=far)
        if c < 3:
            down.start(2 + c)
    take_rows(mo, mo_at)
    near_own, near_pair = rows_of(mo, b), rows_of(mo, 1 - b)
    for c in range(chunks):
        at = slice(c * wide, (c + 1) * wide)
        own_up[c] = dot(near_own, up_ref[:, at]) + dot(near_pair, upp[:, at])
    hs_at = slots(chunks)
    passes = ((0, 1), (2,), (3, 4), (5,))
    for c in range(chunks):
        take(ur.at[c], us_at + c)
        hidden = jnp.maximum(own_up[c] + ur[c].astype(f32), 0.0)
        hs[c] = (hidden * hidden).astype(bf)
        put(hs.at[c], hr.at[c], hs_at + c, fs=far)
        if c < 3:
            down.start(5 + c)
        for i in passes[c]:
            down.pass_on(i)
    down.pass_on(6)
    down.pass_on(7)
    down.settle()

    def project(ref, into, ready):
        first = second = 0.0
        for c in range(chunks):
            if ready is not None:
                take(ref.at[c], ready + c)
            at = slice(c * wide, (c + 1) * wide)
            first = first + dot(ref[c], down_ref[at])
            second = second + dot(ref[c], dnp[at])
        first, second = first.astype(bf), second.astype(bf)
        for k in range(n_tp):
            into[k, b] = first[k * share : (k + 1) * share]
            into[k, 1 - b] = second[k * share : (k + 1) * share]

    def reduced(sent, got, at):
        total = sent[t].astype(f32)
        for k in range(1, n_tp):
            take(got.at[t ^ k], at + k)
            total = total + got[t ^ k].astype(f32)
        return total

    near_at, far_at, back_at = slots(n_tp), slots(n_tp), slots(1)
    project(hs, ds.at[0], None)
    for k in range(1, n_tp):
        put(ds.at[0, t ^ k], fr.at[t], near_at + k, tp=t ^ k)
    project(hr, ds.at[1], hs_at)
    for k in range(1, n_tp):
        put(ds.at[1, t ^ k], fq.at[t], far_at + k, tp=t ^ k)
    fs_[...] = reduced(ds.at[1], fq, far_at).astype(bf)
    put(fs_, fz, back_at, fs=far)
    ff[half] = reduced(ds.at[0], fr, near_at)
    take(fz, back_at)
    ff[1 - half] = fz[...].astype(f32)
    feed = [ff[c // 2, c % 2] for c in range(n_fs)]
    scale = squares(feed)
    for c in range(n_fs):
        out_ref[t, :, c * cols : (c + 1) * cols] = (
            st[c] + feed[c] * scale * gain_d_ref[c]
        ).astype(bf)
    out_at = slots(n_tp)
    gather_rows(out_ref, out_at)
    take_rows(out_ref, out_at)
    for copy in waiting:
        copy.wait_send()
    assert count[0] <= send.shape[0]


def local_fused(
    tokens, pre_attention_gain, query_weight, key_weight, value_weight, output_gate_weight,
    decay_weight, decay_logit_bias, extra_log_decay, head_norm_gain, attention_out_weight,
    post_attention_gain, pre_feedforward_gain, post_feedforward_gain, up_weight, down_weight,
):
    bf, f32 = jnp.bfloat16, jnp.float32
    n_fs, n_tp = lax.axis_size("fs"), lax.axis_size("tp")
    length, width = tokens.shape
    share, cols = length // n_tp, width // n_fs
    qk, v = query_weight.shape[1], value_weight.shape[1]
    units = up_weight.shape[1]
    chunks = 4
    vm = pltpu.VMEM
    block = (n_fs, share, cols)
    two = (2, share, cols)
    act = (chunks, length, units // chunks)
    scratch = [
        vm((n_tp,) + block, bf), vm((n_tp,) + two, bf),
        vm(query_weight.shape, bf), vm(key_weight.shape, bf), vm(decay_weight.shape, bf),
        vm(value_weight.shape, bf), vm(output_gate_weight.shape, bf),
        vm((3, length, qk), f32), vm((2, length, v), bf),
        vm((3, length, qk), f32), vm((2, length, v), bf),
        vm((n_fs,) + attention_out_weight.shape, bf),
        vm((n_tp,) + block, bf), vm((n_tp,) + block, bf), vm(block, f32), vm(block, bf),
        vm((n_tp,) + two, bf), vm((n_tp,) + two, bf),
        vm(up_weight.shape, bf), vm(down_weight.shape, bf),
        vm(act, bf), vm(act, bf), vm(act, bf), vm(act, bf),
        vm((2, n_tp) + two, bf), vm((n_tp,) + two, bf), vm((n_tp,) + two, bf),
        vm(two, bf), vm(two, bf), vm((2,) + two, f32), vm(act, f32),
        pltpu.SemaphoreType.DMA((96,)), pltpu.SemaphoreType.DMA((96,)),
    ]

    def kernel(*refs):
        exchange_kernel(*refs, n_fs=n_fs, n_tp=n_tp, qk=qk, v=v)

    def gain_blocks(gain):
        return gain.reshape(n_fs, 1, cols)

    out = pl.pallas_call(
        kernel,
        out_shape=jax.ShapeDtypeStruct((n_tp, share, width), bf),
        in_specs=[pl.BlockSpec(memory_space=pltpu.VMEM)] * 16,
        out_specs=pl.BlockSpec(memory_space=pltpu.VMEM),
        scratch_shapes=scratch,
        compiler_params=pltpu.CompilerParams(
            collective_id=0, has_side_effects=True, vmem_limit_bytes=60 * 2**20
        ),
    )(
        tokens.reshape(n_tp, share, width), query_weight, key_weight, decay_weight,
        value_weight, output_gate_weight, decay_logit_bias.reshape(1, qk),
        extra_log_decay, head_norm_gain.reshape(1, v), attention_out_weight,
        gain_blocks(pre_attention_gain), gain_blocks(post_attention_gain),
        gain_blocks(pre_feedforward_gain), gain_blocks(post_feedforward_gain),
        up_weight, down_weight,
    )
    return out.reshape(length, width)


def local(*arrays):
    n_fs, n_tp, n_grp = (lax.axis_size(name) for name in ("fs", "tp", "grp"))
    length, width = arrays[0].shape
    fits = n_fs == 4 and n_grp == 2 and n_tp in (2, 4, 8) and width // n_fs % 128 == 0
    fits = fits and length % (n_tp * 16) == 0 and arrays[2].shape[1] % 128 == 0
    fits = fits and arrays[-2].shape[1] % 512 == 0
    return local_fused(*arrays) if fits else local_plain(*arrays)


def solution(mesh):
    return jax.shard_map(
        local,
        mesh=mesh,
        in_specs=(
            P(("grp", "fs"), None), P(), P("fs", "tp"), P("fs", "tp"), P("fs", "tp"),
            P("fs", "tp"), P("fs", "tp"), P("tp"), P(("grp", "fs"), "tp"), P("tp"),
            P("tp", "fs"), P(), P(), P(), P("fs", "tp"), P("tp", "fs"),
        ),
        out_specs=P(("grp", "fs"), None),
        check_vma=False,
    )
```

```python
import jax
import jax.numpy as jnp
from jax import lax
from jax.experimental import pallas as pl
from jax.experimental.pallas import tpu as pltpu
from jax.sharding import PartitionSpec as P

DK = 64
DV = 128
EPS = 1e-06
GATE_NORM_SCALE = 16.0


def root_norm(rows, gain):
    return rows * lax.rsqrt(jnp.mean(rows * rows, axis=-1, keepdims=True) + EPS) * gain


def split2(x):
    hi = x.astype(jnp.bfloat16)
    lo = (x - hi.astype(jnp.float32)).astype(jnp.bfloat16)
    return hi, lo


def dot_t(a, b):
    return lax.dot_general(a, b, (((1,), (1,)), ((), ())), preferred_element_type=jnp.float32)


def split3(x):
    hi = x.astype(jnp.bfloat16)
    rest = x - hi.astype(jnp.float32)
    mid = rest.astype(jnp.bfloat16)
    return hi, mid, (rest - mid.astype(jnp.float32)).astype(jnp.bfloat16)


def pick(mask, parts):
    chosen = mask.astype(jnp.float32).astype(jnp.bfloat16)
    total = 0.0
    for part in parts:
        total = total + jnp.dot(chosen, part, preferred_element_type=jnp.float32)
    return total


def attend(q, k, v, log_decay):
    n, width = q.shape
    heads = width // DK
    row = lax.broadcasted_iota(jnp.int32, (n, n), 0)
    col = lax.broadcasted_iota(jnp.int32, (n, n), 1)
    lane = lax.broadcasted_iota(jnp.int32, (n, width), 1)
    cum = pick(row >= col, split3(log_decay))
    cum_parts = split3(cum)

    def per_head(x):
        return jnp.concatenate(
            [jnp.where((lane >= h * DK) & (lane < (h + 1) * DK), x, 0.0) for h in range(heads)], 0
        )

    def scores_of(left, right):
        lh, ll = split2(per_head(left))
        rh, rl = split2(right)
        return dot_t(lh, rh) + dot_t(lh, rl) + dot_t(ll, rh)

    tiled_row = jnp.concatenate([row] * heads, 0)
    tiled_col = jnp.concatenate([col] * heads, 0)
    scores = jnp.where(
        tiled_row == tiled_col,
        dot_t(per_head(q).astype(jnp.bfloat16), k.astype(jnp.bfloat16)),
        0.0,
    )
    half = n // 2
    while half >= 1:
        bound = pick(col == (row & ~(2 * half - 1)) + (half - 1), cum_parts)
        fade = jnp.exp(-jnp.abs(cum - bound))
        part = scores_of(q * fade, k * fade)
        apart = tiled_row ^ tiled_col
        keep = (apart >= half) & (apart < 2 * half) & (tiled_row > tiled_col)
        scores = jnp.where(keep, part, scores)
        half //= 2
    outs = []
    for h in range(heads):
        sh, sl = split2(scores[h * n : (h + 1) * n])
        vh = v[:, h * DV : (h + 1) * DV]
        outs.append(
            jnp.dot(sh, vh, preferred_element_type=jnp.float32)
            + jnp.dot(sl, vh, preferred_element_type=jnp.float32)
        )
    return outs


def head_block(acc, bias, extra, gain, qk, v):
    bf = jnp.bfloat16
    q = acc[:, :qk].astype(bf).astype(jnp.float32) * DK ** (-0.5)
    k = acc[:, qk : 2 * qk].astype(bf).astype(jnp.float32)
    x = acc[:, 2 * qk : 3 * qk] + bias
    log_sig = jnp.minimum(x, 0.0) - jnp.log1p(jnp.exp(-jnp.abs(x)))
    rate = log_sig / GATE_NORM_SCALE + extra
    vals = acc[:, 3 * qk : 3 * qk + v].astype(bf)
    gate = acc[:, 3 * qk + v :].astype(bf).astype(jnp.float32)
    outs = attend(q, k, vals, rate)
    scaled = jnp.concatenate(
        [o * lax.rsqrt(jnp.mean(o * o, axis=-1, keepdims=True) + EPS) for o in outs], 1
    )
    return (scaled * gain * (gate / (1.0 + jnp.exp(-gate)))).astype(bf)


def local_plain(
    tokens, pre_attention_gain, query_weight, key_weight, value_weight, output_gate_weight,
    decay_weight, decay_logit_bias, extra_log_decay, head_norm_gain, attention_out_weight,
    post_attention_gain, pre_feedforward_gain, post_feedforward_gain, up_weight, down_weight,
):
    bf = jnp.bfloat16
    n_fs = lax.axis_size("fs")
    n_tp = lax.axis_size("tp")
    length, width = tokens.shape
    share = length // n_tp
    cols = width // n_fs
    qk, v = query_weight.shape[1], value_weight.shape[1]
    stream_in = tokens.astype(jnp.float32)
    normed = root_norm(stream_in, pre_attention_gain).astype(bf)
    joined = jnp.concatenate(
        [query_weight, key_weight, decay_weight, value_weight, output_gate_weight], 1
    )
    whole = lax.all_gather(joined, "fs", axis=0, tiled=True)
    acc = jnp.dot(normed, whole, preferred_element_type=jnp.float32)
    headout = head_block(acc, decay_logit_bias, extra_log_decay, head_norm_gain, qk, v)
    whole_out = lax.all_gather(attention_out_weight, "fs", axis=1, tiled=True)
    mix_part = jnp.dot(headout, whole_out, preferred_element_type=jnp.float32).astype(bf)
    mix = lax.all_to_all(
        mix_part.reshape(n_tp, share, width), "tp", split_axis=0, concat_axis=0, tiled=True
    )
    mixed = jnp.sum(mix.astype(jnp.float32), 0)
    mine = lax.dynamic_slice_in_dim(stream_in, lax.axis_index("tp") * share, share, 0)
    stream = mine + root_norm(mixed, post_attention_gain)
    normed_mid = root_norm(stream, pre_feedforward_gain).astype(bf)
    blocks = normed_mid.reshape(share, n_fs, cols).transpose(1, 0, 2)
    blocks = lax.all_to_all(blocks, "fs", split_axis=0, concat_axis=0, tiled=True)
    rows = lax.all_gather(blocks, "tp", axis=1, tiled=True)
    up = jnp.dot(rows.reshape(n_fs * length, cols), up_weight, preferred_element_type=jnp.float32)
    up = up.astype(bf).reshape(n_fs, length, -1)
    up = lax.all_to_all(up, "fs", split_axis=0, concat_axis=0, tiled=True)
    hidden = jnp.square(jax.nn.relu(jnp.sum(up.astype(jnp.float32), 0))).astype(bf)
    hidden = lax.all_gather(hidden, "fs", axis=0, tiled=True)
    down = jnp.dot(hidden, down_weight, preferred_element_type=jnp.float32).astype(bf)
    down = down.reshape(n_fs, n_tp, share, cols).transpose(1, 0, 2, 3)
    down = lax.all_to_all(down, "tp", split_axis=0, concat_axis=0, tiled=True)
    feed = jnp.sum(down.astype(jnp.float32), 0).astype(bf)
    feed = lax.all_to_all(feed, "fs", split_axis=0, concat_axis=0, tiled=True)
    feed = feed.transpose(1, 0, 2).reshape(share, width).astype(jnp.float32)
    out = (stream + root_norm(feed, post_feedforward_gain)).astype(bf)
    return lax.all_gather(out, "tp", axis=0, tiled=True)


def exchange_kernel(
    x_ref, q_ref, k_ref, d_ref, v_ref, g_ref, bias_ref, extra_ref, head_gain_ref, wo_ref,
    gain_a_ref, gain_b_ref, gain_c_ref, gain_d_ref, up_ref, down_ref, out_ref,
    nm, no, qp, kp, dp, vp, gp, p32s, p16s, p32r, p16r, pds, pdr, wop, mixs, mixr, st, mid, mo, mx,
    upp, dnp, us, ur, hs, hr, ds, fr, fq, fs_, fz, ff, own_up, send, recv,
    *, n_fs, n_tp, qk, v,
):
    bf, f32 = jnp.bfloat16, jnp.float32
    g, f, t = lax.axis_index("grp"), lax.axis_index("fs"), lax.axis_index("tp")
    pair, far, b, half = f ^ 1, f ^ 2, f & 1, f >> 1
    share = out_ref.shape[1]
    cols = mid.shape[2]
    length = n_tp * share
    waiting = []
    count = [0]

    def slots(n):
        first = count[0]
        count[0] += n
        return first

    def put(src, dst, at, **where):
        copy = pltpu.make_async_remote_copy(
            src_ref=src, dst_ref=dst, send_sem=send.at[at], recv_sem=recv.at[at],
            device_id=where, device_id_type=pl.DeviceIdType.MESH,
        )
        copy.start()
        waiting.append(copy)

    def take(dst, at):
        pltpu.make_async_remote_copy(
            src_ref=dst, dst_ref=dst, send_sem=send.at[at], recv_sem=recv.at[at],
            device_id={"fs": far}, device_id_type=pl.DeviceIdType.MESH,
        ).wait_recv()

    barrier = pltpu.get_barrier_semaphore()
    peers = [{"grp": 1 - g}]
    peers += [{"fs": f ^ s} for s in range(1, n_fs)]
    peers += [{"tp": t ^ k} for k in range(1, n_tp)]
    for peer in peers:
        pl.semaphore_signal(barrier, inc=1, device_id=peer, device_id_type=pl.DeviceIdType.MESH)
    pl.semaphore_wait(barrier, len(peers))

    class Fetch:
        def __init__(self, ref, into, pieces):
            self.ref, self.into, self.pieces = ref, into, pieces
            self.at = slots(2 * pieces)
            self.size = ref.shape[0] // (2 * pieces)

        def piece(self, ref, part, i):
            at = pl.multiple_of(part * (self.pieces * self.size) + i * self.size, self.size)
            return ref.at[pl.ds(at, self.size)]

        def start(self, i):
            put(self.piece(self.ref, g, i), self.piece(self.into, g, i), self.at + i, fs=pair)

        def pass_on(self, i):
            mine = self.piece(self.into, g, i)
            take(mine, self.at + i)
            put(mine, mine, self.at + self.pieces + i, grp=1 - g)

        def settle(self):
            for i in range(self.pieces):
                take(self.piece(self.into, 1 - g, i), self.at + self.pieces + i)

    def gather_rows(ref, at):
        for k in range(1, n_tp):
            put(ref.at[t], ref.at[t], at + k, tp=t ^ k)

    def take_rows(ref, at):
        for k in range(1, n_tp):
            take(ref.at[t ^ k], at + k)

    def rows_of(ref, at):
        return ref[:, at].reshape(length, cols)

    def dot(l, r):
        return jnp.dot(l, r, preferred_element_type=f32)

    def squares(blocks):
        total = 0.0
        for block in blocks:
            total = total + jnp.sum(block * block, axis=-1, keepdims=True)
        return lax.rsqrt(total / (n_fs * cols) + EPS)

    projections = [Fetch(r, p, 2) for r, p in zip((q_ref, k_ref, d_ref, v_ref, g_ref), (qp, kp, dp, vp, gp))]
    for weight in projections:
        weight.start(0)
        weight.start(1)

    x = [x_ref[:, :, c * cols : (c + 1) * cols].astype(f32) for c in range(n_fs)]
    scale = squares(x)
    for c in range(n_fs):
        nm[:, c] = (x[c] * scale * gain_a_ref[c]).astype(bf)
    no_at = slots(n_tp)
    put(nm.at[t, pl.ds(2 * (1 - half), 2)], no.at[t], no_at, fs=far)

    wo_at = slots(2 * n_fs)
    rows_wo = wo_ref.shape[0] // 2

    def wo_part(ref, part):
        return ref.at[pl.ds(pl.multiple_of(part * rows_wo, rows_wo), rows_wo)]

    for s in (2, 3, 1):
        put(wo_part(wo_ref, g), wo_part(wop.at[f], g), wo_at + s, fs=f ^ s)

    for weight in projections[:2]:
        weight.pass_on(0)
        weight.pass_on(1)
    take(no.at[t], no_at)
    gather_rows(no, no_at)
    for weight in projections[2:]:
        weight.pass_on(0)
        weight.pass_on(1)
    take_rows(no, no_at)

    up = Fetch(up_ref, upp, 4)
    down = Fetch(down_ref, dnp, 8)
    part_at = slots(5)
    no_own, no_pair = rows_of(no, b), rows_of(no, 1 - b)
    outgoing = [p32s.at[0], p32s.at[1], pds, p16s.at[0], p16s.at[1]]
    incoming = [p32r.at[0], p32r.at[1], pdr, p16r.at[0], p16r.at[1]]
    for i, weight in enumerate(projections):
        weight.settle()
        other = dot(no_own, weight.ref[...]) + dot(no_pair, weight.into[...])
        outgoing[i][...] = other.astype(outgoing[i].dtype)
        put(outgoing[i], incoming[i], part_at + i, fs=far)
    for i in range(4):
        up.start(i)
    nm_own, nm_pair = rows_of(nm, f), rows_of(nm, pair)
    acc = [dot(nm_own, w.ref[...]) + dot(nm_pair, w.into[...]) for w in projections]
    for s in (1, 2, 3):
        mine = wo_part(wop.at[f ^ s], g)
        take(mine, wo_at + s)
        put(mine, mine, wo_at + n_fs + s, grp=1 - g)
    for i in range(5):
        take(incoming[i], part_at + i)
        acc[i] = acc[i] + incoming[i][...].astype(f32)
    up.pass_on(0)
    headout = head_block(
        jnp.concatenate(acc, 1), bias_ref[...], extra_ref[...], head_gain_ref[...], qk, v
    )
    for s in (1, 2, 3):
        take(wo_part(wop.at[f ^ s], 1 - g), wo_at + n_fs + s)
    up.pass_on(1)
    for s in range(n_fs):
        weight = wo_ref[...] if s == 0 else wop[f ^ s]
        block = dot(headout, weight).astype(bf)
        for k in range(n_tp):
            mixs[k, f ^ s] = block[k * share : (k + 1) * share]
    mix_at = slots(n_tp)
    for k in range(1, n_tp):
        put(mixs.at[t ^ k], mixr.at[t], mix_at + k, tp=t ^ k)
    up.pass_on(2)
    mix = mixs[t].astype(f32)
    for k in range(1, n_tp):
        take(mixr.at[t ^ k], mix_at + k)
        mix = mix + mixr[t ^ k].astype(f32)
    mix = [mix[c] for c in range(n_fs)]
    scale = squares(mix)
    mine = [x_ref[t, :, c * cols : (c + 1) * cols].astype(f32) for c in range(n_fs)]
    stream = [mine[c] + mix[c] * scale * gain_b_ref[c] for c in range(n_fs)]
    scale = squares(stream)
    for c in range(n_fs):
        st[c] = stream[c]
        mid[c] = (stream[c] * scale * gain_c_ref[c]).astype(bf)
    mx_at, mo_at = slots(n_tp), slots(n_tp)
    put(mid.at[pl.ds(2 * (1 - half), 2)], mx.at[t], mx_at, fs=far)
    for k in range(1, n_tp):
        put(mid.at[pl.ds(2 * half, 2)], mo.at[t], mo_at + k, tp=t ^ k)
    down.start(0)
    down.start(1)
    mo[t, 0] = mid[2 * half]
    mo[t, 1] = mid[2 * half + 1]
    take(mx.at[t], mx_at)
    gather_rows(mx, mx_at)
    up.pass_on(3)
    take_rows(mx, mx_at)
    up.settle()

    chunks = us.shape[0]
    wide = us.shape[2]
    us_at = slots(chunks)
    far_own, far_pair = rows_of(mx, b), rows_of(mx, 1 - b)
    for c in range(chunks):
        at = slice(c * wide, (c + 1) * wide)
        us[c] = (dot(far_own, up_ref[:, at]) + dot(far_pair, upp[:, at])).astype(bf)
        put(us.at[c], ur.at[c], us_at + c, fs=far)
        if c < 3:
            down.start(2 + c)
    take_rows(mo, mo_at)
    near_own, near_pair = rows_of(mo, b), rows_of(mo, 1 - b)
    for c in range(chunks):
        at = slice(c * wide, (c + 1) * wide)
        own_up[c] = dot(near_own, up_ref[:, at]) + dot(near_pair, upp[:, at])
    hs_at = slots(chunks)
    passes = ((0, 1), (2,), (3, 4), (5,))
    for c in range(chunks):
        take(ur.at[c], us_at + c)
        hidden = jnp.maximum(own_up[c] + ur[c].astype(f32), 0.0)
        hs[c] = (hidden * hidden).astype(bf)
        put(hs.at[c], hr.at[c], hs_at + c, fs=far)
        if c < 3:
            down.start(5 + c)
        for i in passes[c]:
            down.pass_on(i)
    down.pass_on(6)
    down.pass_on(7)
    down.settle()

    def project(ref, into, ready):
        first = second = 0.0
        for c in range(chunks):
            if ready is not None:
                take(ref.at[c], ready + c)
            at = slice(c * wide, (c + 1) * wide)
            first = first + dot(ref[c], down_ref[at])
            second = second + dot(ref[c], dnp[at])
        first, second = first.astype(bf), second.astype(bf)
        for k in range(n_tp):
            into[k, b] = first[k * share : (k + 1) * share]
            into[k, 1 - b] = second[k * share : (k + 1) * share]

    def reduced(sent, got, at):
        total = sent[t].astype(f32)
        for k in range(1, n_tp):
            take(got.at[t ^ k], at + k)
            total = total + got[t ^ k].astype(f32)
        return total

    near_at, far_at, back_at = slots(n_tp), slots(n_tp), slots(1)
    project(hs, ds.at[0], None)
    for k in range(1, n_tp):
        put(ds.at[0, t ^ k], fr.at[t], near_at + k, tp=t ^ k)
    project(hr, ds.at[1], hs_at)
    for k in range(1, n_tp):
        put(ds.at[1, t ^ k], fq.at[t], far_at + k, tp=t ^ k)
    fs_[...] = reduced(ds.at[1], fq, far_at).astype(bf)
    put(fs_, fz, back_at, fs=far)
    ff[half] = reduced(ds.at[0], fr, near_at)
    take(fz, back_at)
    ff[1 - half] = fz[...].astype(f32)
    feed = [ff[c // 2, c % 2] for c in range(n_fs)]
    scale = squares(feed)
    for c in range(n_fs):
        out_ref[t, :, c * cols : (c + 1) * cols] = (
            st[c] + feed[c] * scale * gain_d_ref[c]
        ).astype(bf)
    out_at = slots(n_tp)
    gather_rows(out_ref, out_at)
    take_rows(out_ref, out_at)
    for copy in waiting:
        copy.wait_send()
    assert count[0] <= send.shape[0]


def local_fused(
    tokens, pre_attention_gain, query_weight, key_weight, value_weight, output_gate_weight,
    decay_weight, decay_logit_bias, extra_log_decay, head_norm_gain, attention_out_weight,
    post_attention_gain, pre_feedforward_gain, post_feedforward_gain, up_weight, down_weight,
):
    bf, f32 = jnp.bfloat16, jnp.float32
    n_fs, n_tp = lax.axis_size("fs"), lax.axis_size("tp")
    length, width = tokens.shape
    share, cols = length // n_tp, width // n_fs
    qk, v = query_weight.shape[1], value_weight.shape[1]
    units = up_weight.shape[1]
    chunks = 4
    vm = pltpu.VMEM
    block = (n_fs, share, cols)
    two = (2, share, cols)
    act = (chunks, length, units // chunks)
    scratch = [
        vm((n_tp,) + block, bf), vm((n_tp,) + two, bf),
        vm(query_weight.shape, bf), vm(key_weight.shape, bf), vm(decay_weight.shape, bf),
        vm(value_weight.shape, bf), vm(output_gate_weight.shape, bf),
        vm((2, length, qk), f32), vm((2, length, v), bf),
        vm((2, length, qk), f32), vm((2, length, v), bf),
        vm((length, qk), bf), vm((length, qk), bf),
        vm((n_fs,) + attention_out_weight.shape, bf),
        vm((n_tp,) + block, bf), vm((n_tp,) + block, bf), vm(block, f32), vm(block, bf),
        vm((n_tp,) + two, bf), vm((n_tp,) + two, bf),
        vm(up_weight.shape, bf), vm(down_weight.shape, bf),
        vm(act, bf), vm(act, bf), vm(act, bf), vm(act, bf),
        vm((2, n_tp) + two, bf), vm((n_tp,) + two, bf), vm((n_tp,) + two, bf),
        vm(two, bf), vm(two, bf), vm((2,) + two, f32), vm(act, f32),
        pltpu.SemaphoreType.DMA((96,)), pltpu.SemaphoreType.DMA((96,)),
    ]

    def kernel(*refs):
        exchange_kernel(*refs, n_fs=n_fs, n_tp=n_tp, qk=qk, v=v)

    def gain_blocks(gain):
        return gain.reshape(n_fs, 1, cols)

    out = pl.pallas_call(
        kernel,
        out_shape=jax.ShapeDtypeStruct((n_tp, share, width), bf),
        in_specs=[pl.BlockSpec(memory_space=pltpu.VMEM)] * 16,
        out_specs=pl.BlockSpec(memory_space=pltpu.VMEM),
        scratch_shapes=scratch,
        compiler_params=pltpu.CompilerParams(
            collective_id=0, has_side_effects=True, vmem_limit_bytes=60 * 2**20
        ),
    )(
        tokens.reshape(n_tp, share, width), query_weight, key_weight, decay_weight,
        value_weight, output_gate_weight, decay_logit_bias.reshape(1, qk),
        extra_log_decay, head_norm_gain.reshape(1, v), attention_out_weight,
        gain_blocks(pre_attention_gain), gain_blocks(post_attention_gain),
        gain_blocks(pre_feedforward_gain), gain_blocks(post_feedforward_gain),
        up_weight, down_weight,
    )
    return out.reshape(length, width)


def local(*arrays):
    n_fs, n_tp, n_grp = (lax.axis_size(name) for name in ("fs", "tp", "grp"))
    length, width = arrays[0].shape
    fits = n_fs == 4 and n_grp == 2 and n_tp in (2, 4, 8) and width // n_fs % 128 == 0
    fits = fits and length % (n_tp * 16) == 0 and arrays[2].shape[1] % 128 == 0
    fits = fits and arrays[-2].shape[1] % 512 == 0
    return local_fused(*arrays) if fits else local_plain(*arrays)


def solution(mesh):
    return jax.shard_map(
        local,
        mesh=mesh,
        in_specs=(
            P(("grp", "fs"), None), P(), P("fs", "tp"), P("fs", "tp"), P("fs", "tp"),
            P("fs", "tp"), P("fs", "tp"), P("tp"), P(("grp", "fs"), "tp"), P("tp"),
            P("tp", "fs"), P(), P(), P(), P("fs", "tp"), P("tp", "fs"),
        ),
        out_specs=P(("grp", "fs"), None),
        check_vma=False,
    )
```
